32 devices in a mesh: sp: 8 (over z, x), tp: 4 (over y, core).
Axes of the slice: x: 2, y: 2, z: 4, core: 2. Of those that a mesh axis runs over, the one named last changes fastest.
Arguments:
- out_grad: bfloat16 [1024, 2048], P('sp', 'tp'), may hold values from -6 to 6
- moe_input: bfloat16 [1024, 2048], P('sp', 'tp'), may hold values from -6 to 6
- route_weight: float32 [1024, 2], P('sp'), may hold values from 0.2 to 1
- route_ids: int32 [1024, 2], P('sp'), may hold values from 0 to 7, all different within a row; in each aligned block of 128 rows (0 to 127, 128 to 255, ...) at most 64 rows name the same one
- gate_proj: bfloat16 [8, 2048, 2816], P('sp', None, 'tp'), may hold values from -0.125 to 0.125
- up_proj: bfloat16 [8, 2048, 2816], P('sp', None, 'tp'), may hold values from -0.125 to 0.125
- down_proj: bfloat16 [8, 2816, 2048], P('sp', 'tp'), may hold values from -0.109375 to 0.109375
- out_proj: bfloat16 [2048, 2048], P(None, 'tp'), may hold values from -0.125 to 0.125
- conv_out: bfloat16 [1024, 2048], P('sp', 'tp'), may hold values from -6 to 6
- gate_b: bfloat16 [1024, 2048], P('sp', 'tp'), may hold values from -6 to 6
- gate_c: bfloat16 [1024, 2048], P('sp', 'tp'), may hold values from -6 to 6
- value_v: bfloat16 [1024, 2048], P('sp', 'tp'), may hold values from -6 to 6
- conv_taps: float32 [3, 2048], P(None, 'tp'), may hold values from -3 to 3
Outputs:
- grad_gate: bfloat16 [8, 2048, 2816], P('sp', None, 'tp')
- grad_up: bfloat16 [8, 2048, 2816], P('sp', None, 'tp')
- grad_down: bfloat16 [8, 2816, 2048], P('sp', 'tp')
- grad_out: float32 [2048, 2048], P('sp', 'tp')
- grad_b: bfloat16 [1024, 2048], P('sp', 'tp')
- grad_c: bfloat16 [1024, 2048], P('sp', 'tp')
- grad_v: bfloat16 [1024, 2048], P('sp', 'tp')
The draws below stay inside these ranges and needn't reach their ends.
Inputs may be any that keep to these rules, and one draw needn't show every extreme that they name: `route_ids`: each row names two different experts; within the 128 rows of one index of sp no expert is named by more than 64 rows, a bound that some block reaches.
All inputs are finite; a program needn't handle non-finite values.
Results may differ from the reference program's by a relative error of at most 0.019.
Values may be sent and summed in bfloat16 or wider, within the bound.
No kernel may reach another device: no remote copies, remote signals or barrier semaphores. Data moves between devices by JAX's collectives and lax.ppermute only.
A program may use at most 64 MiB of HBM per device.

```python
import math
import jax
import jax.numpy as jnp
import numpy as np
from jax import lax

D = 2048
FF = 2816
TOK_DEV = 128
TOKENS = 1024
EXPERTS = 8
CAP = 64
N_SP = 8
N_TP = 4


def with_spikes(drawn, key, source, target, shards_of, factor):
    owner, partner = [(jnp.arange(drawn.shape[axis_at]) // (drawn.shape[axis_at] // shards_of)).reshape([-1 if axis == axis_at else 1 for axis in range(drawn.ndim)]) for axis_at in (source, target)]
    chosen = jax.random.permutation(key, shards_of)[partner]
    strong = (owner == chosen) | (owner == (partner + shards_of // 2) % shards_of)
    return jnp.where(strong, factor * drawn, drawn)


def block_levels(rng, shape, pieces, smallest, top_value):
    def one(axis_at, blocks):
        heights = jax.random.uniform(jax.random.fold_in(jax.random.fold_in(rng, 6), axis_at), (blocks,), jnp.float32, smallest / len(pieces), top_value / len(pieces))
        return jnp.repeat(jnp.exp(heights), shape[axis_at] // blocks).reshape((-1,) + (1,) * (len(shape) - axis_at - 1))

    level = one(*pieces[0])
    for cut in pieces[1:]:
        level = level * one(*cut)
    return level


def routed_block(key, own, number, rows, amount, top, bound, skew):
    order = jax.random.permutation(key, amount)
    crowded, ordinary = portions_of(amount, rows * top, bound, skew, True), portions_of(amount, rows * top, bound, skew, False)
    places = jnp.arange(amount)

    def named(sizes, rotation):
        used = int((sizes > 0).sum())
        fixed = max(1, used // 4)
        passed = fixed + (places - fixed + rotation * (used - fixed)) % max(1, amount - fixed)
        return jnp.zeros((amount,), jnp.int32).at[order[jnp.where(places < fixed, places, passed)]].set(jnp.asarray(sizes, jnp.int32))

    sizes = jnp.where(number % 4 == 0, named(crowded, number // 4), named(ordinary, number - number // 4 - 1))
    mixed = jax.random.permutation(jax.random.fold_in(own, 3), amount)
    donor, sink = mixed[0:amount // 2 * 2:2], mixed[1:amount // 2 * 2:2]
    room = jnp.minimum(sizes[donor] - 1, bound - sizes[sink]) // 2
    room = jnp.where((donor == order[0]) | (sink == order[0]) | (sizes[sink] == 0), 0, jnp.maximum(room, 0))
    passed = jax.random.randint(jax.random.fold_in(own, 4), (amount // 2,), 0, 1 << 20) % (room + 1)
    sizes = sizes.at[donor].add(-passed).at[sink].add(passed)
    labels = jnp.searchsorted(jnp.cumsum(sizes), jnp.arange(rows * top), side="right").astype(jnp.int32)
    grid = labels.reshape(top, rows).T
    grid = grid[jax.random.permutation(jax.random.fold_in(own, 1), rows)]
    rotation = jax.random.randint(jax.random.fold_in(own, 2), (rows, 1), 0, top)
    return jnp.take_along_axis(grid, (jnp.arange(top)[None, :] + rotation) % top, axis=1)


def portions_of(count, total, most, skew, full):
    weights = [(1 << 20) // math.isqrt(standing ** skew) + 1 for standing in range(1, count + 1)]
    largest = most if full else min(most, max(-(-total // count), total * weights[0] // sum(weights)))
    least = 1 if total - largest >= count - 1 else 0
    given, surplus = [largest] + [least] * (count - 1), total - largest - least * (count - 1)
    while surplus > 0:
        movable = [i for i in range(1, count) if given[i] < largest] or [i for i in range(1, count) if given[i] < most]
        mass, left = sum([weights[i] for i in movable]), surplus
        for i in movable:
            addition = min(most - given[i], max(1, left * weights[i] // mass), surplus)
            given[i] = given[i] + addition
            surplus = surplus - addition
    return np.array(given)


def normal_values(rng, shape, deviation, reach, split=(), kind=jnp.bfloat16):
    loudness = block_levels(rng, shape, split, -0.22, 0.18) if split else 1.0
    values = jax.random.normal(rng, shape, jnp.float32) * deviation * loudness
    return jnp.minimum(jnp.maximum(values, -reach), reach).astype(kind)


def bell_draw_with(rng, extent, spread, limit, pieces, heavy, held_as=jnp.bfloat16):
    array = spread * jax.random.normal(rng, extent, jnp.float32)
    if pieces:
        array = array * block_levels(rng, extent, pieces, -0.22, 0.18)
    return jnp.clip(with_spikes(array, jax.random.fold_in(rng, 3), *heavy), -limit, limit).astype(held_as)


def setup_inputs(seed: int = 0) -> dict:
    arg_keys = jax.random.split(jax.random.key(seed), 14)
    out_grad = bell_draw_with(arg_keys[0], (TOKENS, D), 1.0, 6.0, ((0, 8), (1, 4)), (0, 1, 8, 2.0))
    moe_input = normal_values(arg_keys[1], (TOKENS, D), 1.0, 6.0, ((0, 8), (1, 4)))
    route_weight = jnp.clip(jnp.exp(math.log(1.0) - 1.609438 * jax.random.uniform(arg_keys[2], (TOKENS, 2), jnp.float32) ** block_levels(arg_keys[2], (TOKENS, 2), ((0, 8),), -0.2, 0.2)), 0.2, 1.0)
    route_ids_keys = jax.random.split(jax.random.fold_in(arg_keys[3], 1), TOKENS // TOK_DEV)
    route_ids_turns = jax.random.permutation(jax.random.fold_in(arg_keys[3], 3), TOKENS // TOK_DEV)
    route_ids = jax.vmap(lambda own, number: routed_block(jax.random.fold_in(arg_keys[3], 2), own, number, TOK_DEV, EXPERTS, 2, CAP, 1))(route_ids_keys, route_ids_turns).reshape((TOKENS, 2))
    gate_proj = normal_values(arg_keys[4], (EXPERTS, D, FF), D ** -0.5, 0.125, ((0, 8), (2, 4)))
    up_proj = normal_values(arg_keys[5], (EXPERTS, D, FF), D ** -0.5, 0.125, ((0, 8), (2, 4)))
    down_proj = normal_values(arg_keys[6], (EXPERTS, FF, D), FF ** -0.5, 0.109375, ((0, 8), (1, 4)))
    out_proj = normal_values(arg_keys[7], (D, D), D ** -0.5, 0.125, ((1, 4),))
    conv_out = normal_values(arg_keys[8], (TOKENS, D), 1.0, 6.0, ((0, 8), (1, 4)))
    gate_b = normal_values(arg_keys[9], (TOKENS, D), 1.0, 6.0, ((0, 8), (1, 4)))
    gate_c = normal_values(arg_keys[10], (TOKENS, D), 1.0, 6.0, ((0, 8), (1, 4)))
    value_v = normal_values(arg_keys[11], (TOKENS, D), 1.0, 6.0, ((0, 8), (1, 4)))
    conv_taps = normal_values(arg_keys[12], (3, D), 0.6, 3.0, ((1, 4),), jnp.float32)
    return {"out_grad": out_grad, "moe_input": moe_input, "route_weight": route_weight, "route_ids": route_ids, "gate_proj": gate_proj, "up_proj": up_proj, "down_proj": down_proj, "out_proj": out_proj, "conv_out": conv_out, "gate_b": gate_b, "gate_c": gate_c, "value_v": value_v, "conv_taps": conv_taps}


def slot_table(route_ids):
    flat = route_ids.reshape(N_SP, TOK_DEV * 2).astype(jnp.int32)
    onehot = (flat[:, :, None] == jnp.arange(EXPERTS, dtype=jnp.int32)[None, None, :]).astype(jnp.int32)
    before = jnp.cumsum(onehot, axis=1) - onehot
    slot = jnp.sum(before * onehot, axis=2).astype(jnp.int32)
    return (flat * CAP + slot).astype(jnp.int32)


def place_rows(rows, index):
    return jnp.zeros((EXPERTS * CAP, rows.shape[1]), rows.dtype).at[index].set(rows)


def reference(out_grad, moe_input, route_weight, route_ids, gate_proj, up_proj, down_proj, out_proj, conv_out, gate_b, gate_c, value_v, conv_taps):
    dest = slot_table(route_ids)
    sent = (route_weight[:, :, None] * out_grad.astype(jnp.float32)[:, None, :]).astype(jnp.bfloat16)
    rows_x = jnp.broadcast_to(moe_input[:, None, :], (TOKENS, 2, D)).reshape(N_SP, 2 * TOK_DEV, D)
    rows_dy = sent.reshape(N_SP, 2 * TOK_DEV, D)
    slots_x = jax.vmap(place_rows)(rows_x, dest).reshape(N_SP, EXPERTS, CAP, D)
    slots_dy = jax.vmap(place_rows)(rows_dy, dest).reshape(N_SP, EXPERTS, CAP, D)
    width = FF // N_TP

    def expert(index):
        xin = slots_x[:, index].reshape(N_SP * CAP, D)
        dyin = slots_dy[:, index].reshape(N_SP * CAP, D)
        w_gate = gate_proj[index]
        w_up = up_proj[index]
        w_down = down_proj[index]
        gate = jnp.dot(xin, w_gate, preferred_element_type=jnp.float32)
        upval = jnp.dot(xin, w_up, preferred_element_type=jnp.float32)
        sig = jax.nn.sigmoid(gate)
        act = gate * sig
        hidden = (act * upval).astype(jnp.bfloat16)
        g_down = jnp.dot(hidden.T, dyin, preferred_element_type=jnp.float32).astype(jnp.bfloat16)
        dhid = jnp.dot(dyin, w_down.T, preferred_element_type=jnp.float32)
        dgate = (dhid * upval * (sig * (1.0 + gate * (1.0 - sig)))).astype(jnp.bfloat16)
        dup = (dhid * act).astype(jnp.bfloat16)
        g_gate = jnp.dot(xin.T, dgate, preferred_element_type=jnp.float32).astype(jnp.bfloat16)
        g_up = jnp.dot(xin.T, dup, preferred_element_type=jnp.float32).astype(jnp.bfloat16)
        rows = N_SP * CAP
        part = jnp.einsum('rpf,dpf->prd', dgate.reshape(rows, N_TP, width).astype(jnp.float32),
                          w_gate.reshape(D, N_TP, width).astype(jnp.float32))
        part = part + jnp.einsum('rpf,dpf->prd', dup.reshape(rows, N_TP, width).astype(jnp.float32),
                                 w_up.reshape(D, N_TP, width).astype(jnp.float32))
        part = lax.optimization_barrier(part.astype(jnp.bfloat16)).astype(jnp.float32)
        back = jnp.sum(part, axis=0).astype(jnp.bfloat16)
        return g_gate, g_up, g_down, back

    grad_gate, grad_up, grad_down, backs = lax.map(expert, jnp.arange(EXPERTS, dtype=jnp.int32))
    backs = backs.reshape(EXPERTS, N_SP, CAP, D).transpose(1, 0, 2, 3).reshape(N_SP, EXPERTS * CAP, D)
    picked = jax.vmap(lambda table, index: table[index])(backs, dest)
    moe_grad = jnp.sum(picked.reshape(TOKENS, 2, D).astype(jnp.float32), axis=1)
    grad_h = (out_grad.astype(jnp.float32) + moe_grad).astype(jnp.bfloat16)
    grad_z = jnp.dot(grad_h, out_proj, preferred_element_type=jnp.float32)
    dconv = (grad_z * gate_b.astype(jnp.float32)).astype(jnp.bfloat16)
    grad_b = (grad_z * conv_out.astype(jnp.float32)).astype(jnp.bfloat16)
    padded = jnp.pad(dconv.astype(jnp.float32), ((1, 1), (0, 0)))
    grad_u = conv_taps[0] * padded[2:] + conv_taps[1] * padded[1:-1] + conv_taps[2] * padded[:-2]
    grad_c = (grad_u * value_v.astype(jnp.float32)).astype(jnp.bfloat16)
    grad_v = (grad_u * gate_c.astype(jnp.float32)).astype(jnp.bfloat16)
    mixed = (gate_b.astype(jnp.float32) * conv_out.astype(jnp.float32)).astype(jnp.bfloat16)
    grad_out = jnp.dot(grad_h.T, mixed, preferred_element_type=jnp.float32)
    return grad_gate, grad_up, grad_down, grad_out, grad_b, grad_c, grad_v
```

```python
import functools

import jax
import jax.numpy as jnp
from jax import lax
from jax.experimental import pallas as pl
from jax.experimental.pallas import tpu as pltpu
from jax.sharding import PartitionSpec as P


BF = jnp.bfloat16
F32 = jnp.float32
VMEM = pl.BlockSpec(memory_space=pltpu.VMEM)
SMEM = pl.BlockSpec(memory_space=pltpu.SMEM)


def call(body, name, outs, args, smem=1, flops=0, scratch=()):
    moved = sum(a.size * a.dtype.itemsize for a in args) + sum(
        o.size * o.dtype.itemsize for o in outs
    )
    return pl.pallas_call(
        body,
        name=name,
        out_shape=tuple(outs),
        in_specs=[SMEM] * smem + [VMEM] * (len(args) - smem),
        out_specs=tuple([VMEM] * len(outs)),
        scratch_shapes=list(scratch),
        cost_estimate=pl.CostEstimate(flops=flops, transcendentals=0, bytes_accessed=moved),
        compiler_params=pltpu.CompilerParams(vmem_limit_bytes=48 * 1024 * 1024),
    )(*args)


def shape(dims, dtype=BF):
    return jax.ShapeDtypeStruct(dims, dtype)


def nt(a, b):
    return lax.dot_general(a, b, (((1,), (1,)), ((), ())), preferred_element_type=F32)


def tn(a, b):
    return lax.dot_general(a, b, (((0,), (0,)), ((), ())), preferred_element_type=F32)


def dispatch_body(n_sp, nx, cap, me_ref, ids_ref, w_ref, x_ref, og_ref, sel_ref, *outs):
    nz = n_sp // nx
    tok = x_ref.shape[0]
    z, x = me_ref[0], me_ref[1]
    ids, wts = ids_ref[...], w_ref[...]
    first = lax.broadcasted_iota(jnp.int32, (n_sp, tok), 0)
    rz, rx = first // nx, first % nx
    zz, xx = rz + z, rx + x
    zz = jnp.where(zz >= nz, zz - nz, zz)
    xx = jnp.where(xx >= nx, xx - nx, xx)
    expert = zz * nx + xx
    hit0, hit1 = ids[0:1, :] == expert, ids[1:2, :] == expert
    named = jnp.where(hit0 | hit1, 1.0, 0.0)
    weight = jnp.where(hit0, wts[0:1, :], 0.0) + jnp.where(hit1, wts[1:2, :], 0.0)
    earlier = (
        lax.broadcasted_iota(jnp.int32, (tok, tok), 0)
        < lax.broadcasted_iota(jnp.int32, (tok, tok), 1)
    )
    before = jnp.dot(
        named.astype(BF), jnp.where(earlier, 1.0, 0.0).astype(BF), preferred_element_type=F32
    )
    slot = jnp.where(named > 0.5, before, -1.0)
    place = lax.broadcasted_iota(jnp.int32, (cap, tok), 0).astype(F32)
    xv, og = x_ref[...], og_ref[...]
    for r in range(n_sp):
        take = jnp.where(slot[r : r + 1, :] == place, 1.0, 0.0)
        scale = jnp.sum(take * weight[r : r + 1, :], axis=1, keepdims=True)
        take = take.astype(BF)
        sel_ref[r * cap : (r + 1) * cap, :] = take
        outs[2 * r][...] = jnp.dot(take, xv, preferred_element_type=F32).astype(BF)
        outs[2 * r + 1][...] = (scale * jnp.dot(take, og, preferred_element_type=F32)).astype(BF)


def expert_body(n_b, blk_ref, dst_ref, *refs):
    xs, dys = refs[:n_b], refs[n_b : 2 * n_b]
    wg, wu, wd = refs[2 * n_b : 2 * n_b + 3]
    hid_ref, dg_ref, du_ref = refs[2 * n_b + 3 : 2 * n_b + 6]
    outs = refs[2 * n_b + 6 :]
    ch = xs[0].shape[1]
    gate = up = dhid = None
    for b in range(n_b):
        cols = pl.ds(pl.multiple_of(blk_ref[b] * ch, ch), ch)
        xb, dyb = xs[b][...], dys[b][...]
        g, u, d = nt(xb, wg[:, cols]), nt(xb, wu[:, cols]), nt(dyb, wd[:, cols])
        gate = g if gate is None else gate + g
        up = u if up is None else up + u
        dhid = d if dhid is None else dhid + d
    sig = jax.nn.sigmoid(gate)
    act = gate * sig
    hid_ref[...] = (act * up).astype(BF)
    dg = (dhid * up * (sig * (1.0 + gate * (1.0 - sig)))).astype(BF)
    du = (dhid * act).astype(BF)
    dg_ref[...] = dg
    du_ref[...] = du
    for b in range(n_b):
        cols = pl.ds(pl.multiple_of(dst_ref[b] * ch, ch), ch)
        part = jnp.dot(dg, wg[:, cols], preferred_element_type=F32) + jnp.dot(
            du, wu[:, cols], preferred_element_type=F32
        )
        outs[b][...] = part.astype(BF)


def weight_grad_body(n_g, n_b, blk_ref, *refs):
    lefts, rights, out = refs[:n_g], refs[n_g:-1], refs[-1]
    ch = rights[0].shape[1]
    held = [l[...].T for l in lefts]
    for b in range(n_b):
        total = None
        for g in range(n_g):
            p = jnp.dot(held[g], rights[g * n_b + b][...], preferred_element_type=F32)
            total = p if total is None else total + p
        out[:, pl.ds(pl.multiple_of(blk_ref[b] * ch, ch), ch)] = total.astype(BF)


def add_body(n_out, *refs):
    ins, outs = refs[:-n_out], refs[-n_out:]
    for i in range(n_out):
        outs[i][...] = (ins[2 * i][...].astype(F32) + ins[2 * i + 1][...].astype(F32)).astype(BF)


def sum_split_body(n_in, *refs):
    ins, outs = refs[:n_in], refs[n_in:]
    rows = outs[0].shape[0]
    for i, out in enumerate(outs):
        total = None
        for ref in ins:
            v = ref[i * rows : (i + 1) * rows, :].astype(F32)
            total = v if total is None else total + v
        out[...] = total.astype(BF)


def combine_body(n_sp, sel_ref, og_ref, *refs):
    backs, dh_ref = refs[:n_sp], refs[n_sp]
    cap = backs[0].shape[0]
    rows = jnp.concatenate([b[...] for b in backs], axis=0) if n_sp > 1 else backs[0][...]
    moe = tn(sel_ref[...], rows)
    dh_ref[...] = (og_ref[...].astype(F32) + moe).astype(BF)


def spread_body(n_b, n_sp, blk_ref, tgt_ref, *refs):
    blocks, full_ref, outs = refs[:n_b], refs[n_b], refs[n_b + 1 :]
    ch = blocks[0].shape[1]
    for b in range(n_b):
        full_ref[:, pl.ds(pl.multiple_of(blk_ref[b] * ch, ch), ch)] = blocks[b][...]
    w = outs[0].shape[1]
    lane = 128
    for r in range(n_sp):
        if w % lane == 0:
            outs[r][...] = full_ref[:, pl.ds(pl.multiple_of(tgt_ref[r] * w, lane), w)]
            continue
        fold = lane // w
        wide = full_ref[:, pl.ds(pl.multiple_of(tgt_ref[r] // fold * lane, lane), lane)]
        piece = wide[:, :w]
        for i in range(1, fold):
            piece = jnp.where(tgt_ref[r] % fold == i, wide[:, i * w : (i + 1) * w], piece)
        outs[r][...] = piece


def mixer_body(full_ref, wo_ref, gb_ref, co_ref, dconv_ref, grad_b_ref, first_ref, last_ref):
    dz = jnp.dot(full_ref[...], wo_ref[...], preferred_element_type=F32)
    dconv = (dz * gb_ref[...].astype(F32)).astype(BF)
    dconv_ref[...] = dconv
    grad_b_ref[...] = (dz * co_ref[...].astype(F32)).astype(BF)
    rows = dconv.shape[0]
    first_ref[...] = dconv[0:1, :]
    last_ref[...] = dconv[rows - 1 : rows, :]


def conv_body(dconv_ref, low_ref, high_ref, taps_ref, v_ref, c_ref, gc_ref, gv_ref):
    mid = dconv_ref[...].astype(F32)
    rows = mid.shape[0]
    at = lax.broadcasted_iota(jnp.int32, mid.shape, 0)
    prev = jnp.where(at == 0, low_ref[...].astype(F32), pltpu.roll(mid, 1, 0))
    succ = jnp.where(at == rows - 1, high_ref[...].astype(F32), pltpu.roll(mid, rows - 1, 0))
    taps = taps_ref[...]
    du = taps[0:1, :] * succ + taps[1:2, :] * mid + taps[2:3, :] * prev
    gc_ref[...] = (du * v_ref[...].astype(F32)).astype(BF)
    gv_ref[...] = (du * c_ref[...].astype(F32)).astype(BF)


def grad_out_body(n_sp, *refs):
    lefts, rights, out = refs[:n_sp], refs[n_sp : 2 * n_sp], refs[-1]
    left = jnp.concatenate([l[...] for l in lefts], axis=0)
    right = jnp.concatenate([r[...] for r in rights], axis=0)
    out[...] = tn(left, right)


def local(
    out_grad,
    moe_input,
    route_weight,
    route_ids,
    gate_proj,
    up_proj,
    down_proj,
    out_proj,
    conv_out,
    gate_b,
    gate_c,
    value_v,
    conv_taps,
):
    tok, ch = out_grad.shape
    n_sp, n_tp = lax.axis_size("sp"), lax.axis_size("tp")
    cap = 4 * tok // n_sp
    ny = n_tp // 2
    nx = ny if n_sp % ny == 0 else 1
    nz = n_sp // nx
    me, mt = lax.axis_index("sp"), lax.axis_index("tp")
    z, x, y, c = me // nx, me % nx, mt // 2, mt % 2
    i32 = functools.partial(jnp.asarray, dtype=jnp.int32)

    def sp_perm(rz, rx):
        return [
            (i, ((i // nx + rz) % nz) * nx + (i % nx + rx) % nx) for i in range(n_sp)
        ]

    def send_sp(v, rz, rx):
        return lax.ppermute(v, "sp", sp_perm(rz, rx)) if (rz % nz or rx % nx) else v

    def send_y(v, jy):
        return lax.ppermute(
            v, "tp", [(k, ((k // 2 + jy) % ny) * 2 + k % 2) for k in range(n_tp)]
        )

    def send_core(v):
        return lax.ppermute(v, "tp", [(k, k ^ 1) for k in range(n_tp)])

    def gather_tp(v):
        blocks = []
        for jy in range(ny):
            b = send_y(v, jy) if jy else v
            blocks += [b, send_core(b)]
        return blocks

    rel = [(rz, rx) for rz in range(nz) for rx in range(nx)]
    blk = i32([0]) + jnp.stack(
        [((y - jy) % ny) * 2 + (c + cc) % 2 for jy in range(ny) for cc in range(2)]
    ).astype(jnp.int32)
    dst = jnp.stack(
        [((y + jy) % ny) * 2 + (c + cc) % 2 for jy in range(ny) for cc in range(2)]
    ).astype(jnp.int32)
    tgt = jnp.stack([((z + rz) % nz) * nx + (x + rx) % nx for rz, rx in rel]).astype(jnp.int32)

    outs = call(
        functools.partial(dispatch_body, n_sp, nx, cap),
        "dispatch",
        [shape((n_sp * cap, tok))] + [shape((cap, ch))] * (2 * n_sp),
        [jnp.stack([z, x]).astype(jnp.int32), route_ids.T, route_weight.T, moe_input, out_grad],
        flops=4 * n_sp * cap * tok * ch,
    )
    sel, sent = outs[0], outs[1:]
    n_g = 2 if n_sp % 2 == 0 else 1
    per = n_sp // n_g
    x_blocks, dy_blocks = [], []
    for g in range(n_g):
        mine = rel[g * per : (g + 1) * per]
        got = [
            [send_sp(sent[2 * (g * per + i) + which], rz, rx) for i, (rz, rx) in enumerate(mine)]
            for which in range(2)
        ]
        xg = jnp.concatenate(got[0], axis=0)
        dyg = jnp.concatenate(got[1], axis=0)
        x_blocks.append(gather_tp(xg))
        dy_blocks.append(gather_tp(dyg))

    mixed = (gate_b.astype(F32) * conv_out.astype(F32)).astype(BF)
    mixed = lax.optimization_barrier((mixed, dy_blocks[-1][0]))[0]
    row = [send_sp(mixed, 0, rx) for rx in range(nx)]
    mixed_all = list(row)
    for _ in range(1, nz):
        row = [send_sp(m, 1, 0) for m in row]
        mixed_all += row

    w_gate, w_up, w_down = gate_proj[0].T, up_proj[0].T, down_proj[0]
    ff = w_gate.shape[0]
    rows = per * cap
    hid, dgs, dus, backs = [], [], [], []
    for g in range(n_g):
        outs = call(
            functools.partial(expert_body, n_tp),
            f"expert{g}",
            [shape((rows, ff))] * 3 + [shape((rows, ch))] * n_tp,
            [blk, dst, *x_blocks[g], *dy_blocks[g], w_gate, w_up, w_down],
            smem=2,
            flops=10 * rows * ff * ch * n_tp,
        )
        hid.append(outs[0])
        dgs.append(outs[1])
        dus.append(outs[2])
        parts = outs[3:]
        theirs = [send_core(parts[2 * jy + 1]) for jy in range(ny)]
        pairs = [v for jy in range(ny) for v in (parts[2 * jy], theirs[jy])]
        summed = call(
            functools.partial(add_body, ny), f"pair{g}", [shape((rows, ch))] * ny, pairs, smem=0,
            flops=ny * rows * ch,
        )
        arrived = [summed[0]] + [send_y(summed[jy], jy) for jy in range(1, ny)]
        pieces = call(
            functools.partial(sum_split_body, ny), f"sum{g}", [shape((cap, ch))] * per, arrived,
            smem=0, flops=ny * rows * ch,
        )
        for i, (rz, rx) in enumerate(rel[g * per : (g + 1) * per]):
            backs.append(send_sp(pieces[i], -rz, -rx))

    def weight_grad(name, lefts, rights):
        return call(
            functools.partial(weight_grad_body, n_g, n_tp),
            name,
            [shape((ff, ch * n_tp))],
            [blk, *lefts, *[b for group in rights for b in group]],
            flops=2 * n_g * rows * ff * ch * n_tp,
        )[0]

    grad_down = weight_grad("grad_down", hid, dy_blocks)
    grad_gate = weight_grad("grad_gate", dgs, x_blocks).T
    grad_up = weight_grad("grad_up", dus, x_blocks).T

    dh = call(
        functools.partial(combine_body, n_sp), "combine", [shape((tok, ch))],
        [sel, out_grad, *backs], smem=0, flops=2 * n_sp * cap * tok * ch,
    )[0]
    dh_blocks = gather_tp(dh)
    width = ch * n_tp // n_sp
    outs = call(
        functools.partial(spread_body, n_tp, n_sp), "spread",
        [shape((tok, ch * n_tp))] + [shape((tok, width))] * n_sp,
        [blk, tgt, *dh_blocks], smem=2, flops=tok * ch * n_tp,
    )
    full_h, slices = outs[0], outs[1:]
    dh_all = [send_sp(slices[i], rz, rx) for i, (rz, rx) in enumerate(rel)]

    dconv, grad_b, first, last = call(
        mixer_body, "mixer", [shape((tok, ch)), shape((tok, ch)), shape((1, ch)), shape((1, ch))],
        [full_h, out_proj, gate_b, conv_out], smem=0, flops=2 * tok * ch * ch * n_tp,
    )
    up_pairs = [(i, i + 1) for i in range(n_sp - 1)]
    low = lax.ppermute(last, "sp", up_pairs)
    high = lax.ppermute(first, "sp", [(b, a) for a, b in up_pairs])
    grad_c, grad_v = call(
        conv_body, "conv", [shape((tok, ch))] * 2,
        [dconv, low, high, conv_taps, value_v, gate_c], smem=0, flops=8 * tok * ch,
    )
    grad_out = call(
        functools.partial(grad_out_body, n_sp), "grad_out", [shape((width, ch), F32)],
        [*dh_all, *mixed_all], smem=0, flops=2 * n_sp * tok * width * ch,
    )[0]
    return (grad_gate[None], grad_up[None], grad_down[None], grad_out, grad_b, grad_c, grad_v)


def solution(mesh):
    in_specs = (
        P("sp", "tp"),
        P("sp", "tp"),
        P("sp", None),
        P("sp", None),
        P("sp", None, "tp"),
        P("sp", None, "tp"),
        P("sp", "tp", None),
        P(None, "tp"),
        P("sp", "tp"),
        P("sp", "tp"),
        P("sp", "tp"),
        P("sp", "tp"),
        P(None, "tp"),
    )
    out_specs = (
        P("sp", None, "tp"),
        P("sp", None, "tp"),
        P("sp", "tp", None),
        P("sp", "tp"),
        P("sp", "tp"),
        P("sp", "tp"),
        P("sp", "tp"),
    )
    return jax.shard_map(local, mesh=mesh, in_specs=in_specs, out_specs=out_specs, check_vma=False)
```

```python
import functools
import math

import jax
import jax.numpy as jnp
from jax import lax
from jax.experimental import pallas as pl
from jax.experimental.pallas import tpu as pltpu
from jax.sharding import PartitionSpec as P


EXPERT_MIB, GRAD_MIB = 16, 14
BF = jnp.bfloat16
F32 = jnp.float32
VMEM = pl.BlockSpec(memory_space=pltpu.VMEM)
SMEM = pl.BlockSpec(memory_space=pltpu.SMEM)
HBM = pl.BlockSpec(memory_space=pltpu.HBM)


def call(body, outs, args, smem=1, flops=0, scratch=(), vmem=8, hbm=()):
    args = [
        pltpu.with_memory_space_constraint(a, pltpu.HBM) if i in hbm else a
        for i, a in enumerate(args)
    ]
    moved = sum(a.size * a.dtype.itemsize for a in args) + sum(
        math.prod(o.shape) * o.dtype.itemsize for o in outs
    )
    return pl.pallas_call(
        body,
        out_shape=tuple(outs),
        in_specs=[SMEM if i < smem else HBM if i in hbm else VMEM for i in range(len(args))],
        out_specs=tuple([VMEM] * len(outs)),
        scratch_shapes=list(scratch),
        cost_estimate=pl.CostEstimate(flops=flops, transcendentals=0, bytes_accessed=moved),
        compiler_params=pltpu.CompilerParams(vmem_limit_bytes=vmem * 1024 * 1024),
    )(*args)


def shape(dims, dtype=BF):
    return jax.ShapeDtypeStruct(dims, dtype)


def nt(a, b):
    return lax.dot_general(a, b, (((1,), (1,)), ((), ())), preferred_element_type=F32)


def tn(a, b):
    return lax.dot_general(a, b, (((0,), (0,)), ((), ())), preferred_element_type=F32)


def routing(n_sp, nx, z, x, ids, wts):
    nz = n_sp // nx
    tok = ids.shape[1]
    first = lax.broadcasted_iota(jnp.int32, (n_sp, tok), 0)
    rz, rx = first // nx, first % nx
    zz, xx = rz + z, rx + x
    zz = jnp.where(zz >= nz, zz - nz, zz)
    xx = jnp.where(xx >= nx, xx - nx, xx)
    expert = zz * nx + xx
    hit0, hit1 = ids[0:1, :] == expert, ids[1:2, :] == expert
    named = jnp.where(hit0 | hit1, 1.0, 0.0)
    weight = 0.0
    if wts is not None:
        weight = jnp.where(hit0, wts[0:1, :], 0.0) + jnp.where(hit1, wts[1:2, :], 0.0)
    earlier = (
        lax.broadcasted_iota(jnp.int32, (tok, tok), 0)
        < lax.broadcasted_iota(jnp.int32, (tok, tok), 1)
    )
    before = jnp.dot(
        named.astype(BF), jnp.where(earlier, 1.0, 0.0).astype(BF), preferred_element_type=F32
    )
    return jnp.where(named > 0.5, before, -1.0), weight


def select_body(n_sp, nx, cap, me_ref, ids_ref, sel_ref):
    slot, _ = routing(n_sp, nx, me_ref[0], me_ref[1], ids_ref[...], None)
    place = lax.broadcasted_iota(jnp.int32, (cap, slot.shape[1]), 0).astype(F32)
    for r in range(n_sp):
        take = jnp.where(slot[r : r + 1, :] == place, 1.0, 0.0)
        sel_ref[r * cap : (r + 1) * cap, :] = take.astype(BF)


def dispatch_body(n_sp, nx, cap, me_ref, *refs):
    far, outs, near, sems = refs[:4], refs[4 : 4 + n_sp], refs[4 + n_sp : 8 + n_sp], refs[-1]
    copies = [pltpu.make_async_copy(f, n, sems.at[i]) for i, (f, n) in enumerate(zip(far, near))]
    for copy in copies:
        copy.start()
    for copy in copies:
        copy.wait()
    ids_ref, w_ref, x_ref, og_ref = near
    slot, weight = routing(n_sp, nx, me_ref[0], me_ref[1], ids_ref[...], w_ref[...])
    tok = x_ref.shape[0]
    place = lax.broadcasted_iota(jnp.int32, (cap, tok), 0).astype(F32)
    xv, og = x_ref[...], og_ref[...]
    for r in range(n_sp):
        take = jnp.where(slot[r : r + 1, :] == place, 1.0, 0.0)
        scale = jnp.sum(take * weight[r : r + 1, :], axis=1, keepdims=True)
        take = take.astype(BF)
        outs[r][:cap, :] = jnp.dot(take, xv, preferred_element_type=F32).astype(BF)
        outs[r][cap:, :] = (scale * jnp.dot(take, og, preferred_element_type=F32)).astype(BF)


def rows_of(refs, cap, which):
    return jnp.concatenate(
        [
            ref[at + which * cap : at + (which + 1) * cap, :]
            for ref in refs
            for at in range(0, ref.shape[0], 2 * cap)
        ],
        axis=0,
    )


def load_body(wg, wu, wd, wg_out, wu_out, wd_out, sems):
    pairs = [(wg, wg_out), (wu, wu_out), (wd, wd_out)]
    half = wg.shape[0] // 16 * 8
    rows = wg.shape[0]
    copies = []
    for i, (f, n) in enumerate(pairs):
        for j, (lo, hi) in enumerate(((0, half), (half, rows))):
            copies.append(
                pltpu.make_async_copy(f.at[lo:hi, :], n.at[lo:hi, :], sems.at[2 * i + j])
            )
    for copy in copies:
        copy.start()
    for copy in copies:
        copy.wait()


def mix_body(gb, co, mixed_ref, gb_near, co_near, sems):
    copies = [
        pltpu.make_async_copy(gb, gb_near, sems.at[0]),
        pltpu.make_async_copy(co, co_near, sems.at[1]),
    ]
    for copy in copies:
        copy.start()
    for copy in copies:
        copy.wait()
    mixed_ref[...] = (gb_near[...].astype(F32) * co_near[...].astype(F32)).astype(BF)


def expert_body(n_b, n_g, cap, blk_ref, dst_ref, *refs):
    blocks, refs = refs[: n_b * n_g], refs[n_b * n_g :]
    wg, wu, wd, hid_ref, dg_ref, du_ref = refs[:6]
    outs = refs[6:]
    ch = blocks[0].shape[1]
    gate = up = dhid = None
    for b in range(n_b):
        cols = pl.ds(pl.multiple_of(blk_ref[b] * ch, ch), ch)
        xb, dyb = rows_of(blocks[b::n_b], cap, 0), rows_of(blocks[b::n_b], cap, 1)
        g, u, d = nt(xb, wg[:, cols]), nt(xb, wu[:, cols]), nt(dyb, wd[:, cols])
        gate = g if gate is None else gate + g
        up = u if up is None else up + u
        dhid = d if dhid is None else dhid + d
    sig = jax.nn.sigmoid(gate)
    act = gate * sig
    hid_ref[...] = (act * up).astype(BF)
    dg = (dhid * up * (sig * (1.0 + gate * (1.0 - sig)))).astype(BF)
    du = (dhid * act).astype(BF)
    dg_ref[...] = dg
    du_ref[...] = du
    for b in range(n_b):
        cols = pl.ds(pl.multiple_of(dst_ref[b] * ch, ch), ch)
        part = jnp.dot(dg, wg[:, cols], preferred_element_type=F32) + jnp.dot(
            du, wu[:, cols], preferred_element_type=F32
        )
        outs[b][...] = part.astype(BF)


def weight_grad_body(n_c, n_b, cap, which, blk_ref, *refs):
    lefts, rights, out = refs[:n_c], refs[n_c:-1], refs[-1]
    ch = rights[0].shape[1]
    held = jnp.concatenate([l[...] for l in lefts], axis=0).T
    for b in range(n_b):
        total = jnp.dot(held, rows_of(rights[b::n_b], cap, which), preferred_element_type=F32)
        out[:, pl.ds(pl.multiple_of(blk_ref[b] * ch, ch), ch)] = total.astype(BF)


def add_body(n_out, *refs):
    ins, outs = refs[:-n_out], refs[-n_out:]
    for i in range(n_out):
        outs[i][...] = (ins[2 * i][...].astype(F32) + ins[2 * i + 1][...].astype(F32)).astype(BF)


def sum_split_body(n_in, *refs):
    ins, outs = refs[:n_in], refs[n_in:]
    rows = outs[0].shape[0]
    for i, out in enumerate(outs):
        total = None
        for ref in ins:
            v = ref[i * rows : (i + 1) * rows, :].astype(F32)
            total = v if total is None else total + v
        out[...] = total.astype(BF)


def combine_body(n_sp, sel_ref, og_ref, *refs):
    backs, dh_ref = refs[:n_sp], refs[n_sp]
    rows = jnp.concatenate([b[...] for b in backs], axis=0) if n_sp > 1 else backs[0][...]
    moe = tn(sel_ref[...], rows)
    dh_ref[...] = (og_ref[...].astype(F32) + moe).astype(BF)


def spread_body(n_b, n_sp, blk_ref, tgt_ref, *refs):
    blocks, full_ref, outs = refs[:n_b], refs[n_b], refs[n_b + 1 :]
    ch = blocks[0].shape[1]
    for b in range(n_b):
        full_ref[:, pl.ds(pl.multiple_of(blk_ref[b] * ch, ch), ch)] = blocks[b][...]
    rows, w = full_ref.shape[0], outs[0].shape[1]
    nx, lane = len(outs), 128
    for r in range(n_sp):
        out = outs[r % nx].at[r // nx * rows : (r // nx + 1) * rows, :]
        if w % lane == 0:
            out[...] = full_ref[:, pl.ds(pl.multiple_of(tgt_ref[r] * w, lane), w)]
            continue
        fold = lane // w
        wide = full_ref[:, pl.ds(pl.multiple_of(tgt_ref[r] // fold * lane, lane), lane)]
        piece = wide[:, :w]
        for i in range(1, fold):
            piece = jnp.where(tgt_ref[r] % fold == i, wide[:, i * w : (i + 1) * w], piece)
        out[...] = piece


def regroup_body(nx, *refs):
    ins, outs = refs[:nx], refs[nx:]
    rows = outs[0].shape[0] // nx
    for rz, out in enumerate(outs):
        for rx, ref in enumerate(ins):
            out[rx * rows : (rx + 1) * rows, :] = ref[rz * rows : (rz + 1) * rows, :]


def mixer_body(full_ref, wo_ref, gb_ref, co_ref, dconv_ref, grad_b_ref, first_ref, last_ref):
    dz = jnp.dot(full_ref[...], wo_ref[...], preferred_element_type=F32)
    dconv = (dz * gb_ref[...].astype(F32)).astype(BF)
    dconv_ref[...] = dconv
    grad_b_ref[...] = (dz * co_ref[...].astype(F32)).astype(BF)
    rows = dconv.shape[0]
    first_ref[...] = dconv[0:1, :]
    last_ref[...] = dconv[rows - 1 : rows, :]


def conv_body(dconv_ref, low_ref, high_ref, taps_ref, v_ref, c_ref, gc_ref, gv_ref):
    mid = dconv_ref[...].astype(F32)
    rows = mid.shape[0]
    at = lax.broadcasted_iota(jnp.int32, mid.shape, 0)
    prev = jnp.where(at == 0, low_ref[...].astype(F32), pltpu.roll(mid, 1, 0))
    succ = jnp.where(at == rows - 1, high_ref[...].astype(F32), pltpu.roll(mid, rows - 1, 0))
    taps = taps_ref[...]
    du = taps[0:1, :] * succ + taps[1:2, :] * mid + taps[2:3, :] * prev
    gc_ref[...] = (du * v_ref[...].astype(F32)).astype(BF)
    gv_ref[...] = (du * c_ref[...].astype(F32)).astype(BF)


def grad_out_body(nz, *refs):
    lefts, rights, out = refs[:nz], refs[nz:-1], refs[-1]
    left = jnp.concatenate([l[...] for l in lefts], axis=0)
    right = jnp.concatenate([r[...] for r in rights], axis=0)
    out[...] = tn(left, right)


def grid(n_sp, n_tp):
    ny = n_tp // 2
    nx = ny if n_sp % ny == 0 else 1
    return n_sp // nx, nx, ny


def local(
    out_grad,
    moe_input,
    route_weight,
    route_ids,
    gate_proj,
    up_proj,
    down_proj,
    out_proj,
    conv_out,
    gate_b,
    gate_c,
    value_v,
    conv_taps,
):
    tok, ch = out_grad.shape
    n_sp, n_tp = lax.axis_size("sp"), lax.axis_size("tp")
    cap = 4 * tok // n_sp
    nz, nx, ny = grid(n_sp, n_tp)
    me, mt = lax.axis_index("sp"), lax.axis_index("tp")
    z, x, y, c = me // nx, me % nx, mt // 2, mt % 2
    i32 = functools.partial(jnp.asarray, dtype=jnp.int32)

    def sp_perm(rz, rx):
        return [
            (i, ((i // nx + rz) % nz) * nx + (i % nx + rx) % nx) for i in range(n_sp)
        ]

    def send_sp(v, rz, rx):
        if rz % nz == 0 and rx % nx == 0:
            return v
        return lax.ppermute(v, "sp", sp_perm(rz, rx))

    def send_y(v, jy):
        return lax.ppermute(v, "tp", [(k, ((k // 2 + jy) % ny) * 2 + k % 2) for k in range(n_tp)])

    def send_core(v):
        return lax.ppermute(v, "tp", [(k, k ^ 1) for k in range(n_tp)])

    def gather_tp(v):
        blocks = []
        for jy in range(ny):
            b = send_y(v, jy) if jy else v
            blocks += [b, send_core(b)]
        return blocks

    rel = [(rz, rx) for rz in range(nz) for rx in range(nx)]
    blk = i32([0]) + jnp.stack(
        [((y - jy) % ny) * 2 + (c + cc) % 2 for jy in range(ny) for cc in range(2)]
    ).astype(jnp.int32)
    dst = jnp.stack(
        [((y + jy) % ny) * 2 + (c + cc) % 2 for jy in range(ny) for cc in range(2)]
    ).astype(jnp.int32)
    tgt = jnp.stack([((z + rz) % nz) * nx + (x + rx) % nx for rz, rx in rel]).astype(jnp.int32)

    near = [
        pltpu.VMEM((2, tok), jnp.int32), pltpu.VMEM((2, tok), F32),
        pltpu.VMEM((tok, ch), BF), pltpu.VMEM((tok, ch), BF), pltpu.SemaphoreType.DMA((4,)),
    ]
    at = jnp.stack([z, x]).astype(jnp.int32)
    sent = call(
        functools.partial(dispatch_body, n_sp, nx, cap),
        [shape((2 * cap, ch))] * n_sp,
        [at, route_ids.T, route_weight.T, moe_input, out_grad],
        flops=4 * n_sp * cap * tok * ch, scratch=near, hbm=(1, 2, 3, 4),
    )
    groups = []
    for rz in range(nz):
        got = [send_sp(sent[rz * nx + rx], rz, rx) for rx in range(nx)]
        groups.append(gather_tp(jnp.concatenate(got, axis=0)))

    ff = down_proj.shape[1]
    weights = [gate_proj[0].T, up_proj[0].T, down_proj[0]]
    mixed = call(
        mix_body, [shape((tok, ch))], [gate_b, conv_out], smem=0, hbm=range(2),
        flops=tok * ch,
        scratch=[pltpu.VMEM((tok, ch), BF)] * 2 + [pltpu.SemaphoreType.DMA((2,))],
    )[0]
    weights = call(
        load_body, [shape((ff, ch * n_tp))] * 3, weights, smem=0, hbm=range(3),
        scratch=[pltpu.SemaphoreType.DMA((6,))],
    )
    row = jnp.concatenate([send_sp(mixed, 0, rx) for rx in range(nx)], axis=0)
    mixed_all = [row]
    for _ in range(1, nz):
        row = send_sp(row, 1, 0)
        mixed_all.append(row)

    n_c = 2 if nz % 2 == 0 else 1
    gpc, per = nz // n_c, n_sp // n_c
    rows = per * cap
    hid, dgs, dus, backs = [], [], [], []
    for g in range(n_c):
        outs = call(
            functools.partial(expert_body, n_tp, gpc, cap),
            [shape((rows, ff))] * 3 + [shape((rows, ch))] * n_tp,
            [blk, dst, *[b for group in groups[g * gpc : (g + 1) * gpc] for b in group],
             *weights],
            smem=2, vmem=EXPERT_MIB,
            flops=10 * rows * ff * ch * n_tp,
        )
        blk = lax.optimization_barrier((blk, outs[0]))[0]
        hid.append(outs[0])
        dgs.append(outs[1])
        dus.append(outs[2])
        parts = outs[3:]
        theirs = [send_core(parts[2 * jy + 1]) for jy in range(ny)]
        pairs = [v for jy in range(ny) for v in (parts[2 * jy], theirs[jy])]
        summed = call(
            functools.partial(add_body, ny), [shape((rows, ch))] * ny, pairs, smem=0,
            flops=ny * rows * ch,
        )
        arrived = [summed[0]] + [send_y(summed[jy], jy) for jy in range(1, ny)]
        pieces = call(
            functools.partial(sum_split_body, ny), [shape((cap, ch))] * per, arrived,
            smem=0, flops=ny * rows * ch,
        )
        for i, (rz, rx) in enumerate(rel[g * per : (g + 1) * per]):
            backs.append(send_sp(pieces[i], -rz, -rx))

    def weight_grad(lefts, which):
        return call(
            functools.partial(weight_grad_body, n_c, n_tp, cap, which),
            [shape((ff, ch * n_tp))],
            [blk, *lefts, *[b for group in groups for b in group]],
            flops=2 * n_sp * cap * ff * ch * n_tp, vmem=GRAD_MIB,
        )[0]

    grad_down = weight_grad(hid, 1)
    grad_gate = weight_grad(dgs, 0)
    grad_up = weight_grad(dus, 0)
    *backs, grad_down, grad_gate, grad_up = lax.optimization_barrier(
        (*backs, grad_down, grad_gate, grad_up)
    )
    grad_gate, grad_up = grad_gate.T, grad_up.T

    sel = call(
        functools.partial(select_body, n_sp, nx, cap), [shape((n_sp * cap, tok))],
        [at, route_ids.T], flops=2 * n_sp * cap * tok * tok,
    )[0]
    dh = call(
        functools.partial(combine_body, n_sp), [shape((tok, ch))],
        [sel, out_grad, *backs], smem=0, flops=2 * n_sp * cap * tok * ch,
    )[0]
    dh_blocks = gather_tp(dh)
    width = ch * n_tp // n_sp
    outs = call(
        functools.partial(spread_body, n_tp, n_sp),
        [shape((tok, ch * n_tp))] + [shape((nz * tok, width))] * nx,
        [blk, tgt, *dh_blocks], smem=2, flops=tok * ch * n_tp,
    )
    full_h, slices = outs[0], outs[1:]
    slices = [send_sp(slices[rx], 0, rx) for rx in range(nx)]
    slices = call(
        functools.partial(regroup_body, nx), [shape((nx * tok, width))] * nz, slices,
        smem=0, flops=tok * width,
    )
    dh_all = [send_sp(slices[rz], rz, 0) for rz in range(nz)]

    dconv, grad_b, first, last = call(
        mixer_body, [shape((tok, ch)), shape((tok, ch)), shape((1, ch)), shape((1, ch))],
        [full_h, out_proj, gate_b, conv_out], smem=0, flops=2 * tok * ch * ch * n_tp,
    )
    up_pairs = [(i, i + 1) for i in range(n_sp - 1)]
    low = lax.ppermute(last, "sp", up_pairs)
    high = lax.ppermute(first, "sp", [(b, a) for a, b in up_pairs])
    grad_c, grad_v = call(
        conv_body, [shape((tok, ch))] * 2,
        [dconv, low, high, conv_taps, value_v, gate_c], smem=0, flops=8 * tok * ch,
    )
    grad_out = call(
        functools.partial(grad_out_body, nz), [shape((width, ch), F32)],
        [*dh_all, *mixed_all], smem=0, flops=2 * n_sp * tok * width * ch,
    )[0]
    return (grad_gate[None], grad_up[None], grad_down[None], grad_out, grad_b, grad_c, grad_v)


def solution(mesh):
    in_specs = (
        P("sp", "tp"),
        P("sp", "tp"),
        P("sp", None),
        P("sp", None),
        P("sp", None, "tp"),
        P("sp", None, "tp"),
        P("sp", "tp", None),
        P(None, "tp"),
        P("sp", "tp"),
        P("sp", "tp"),
        P("sp", "tp"),
        P("sp", "tp"),
        P(None, "tp"),
    )
    out_specs = (
        P("sp", None, "tp"),
        P("sp", None, "tp"),
        P("sp", "tp", None),
        P("sp", "tp"),
        P("sp", "tp"),
        P("sp", "tp"),
        P("sp", "tp"),
    )
    return jax.shard_map(local, mesh=mesh, in_specs=in_specs, out_specs=out_specs, check_vma=False)
```

```python
import functools
import math

import jax
import jax.numpy as jnp
from jax import lax
from jax.experimental import pallas as pl
from jax.experimental.pallas import tpu as pltpu
from jax.sharding import PartitionSpec as P


EXPERT_MIB, GRAD_MIB = 16, 14
LOAD_CUTS = 4
BF = jnp.bfloat16
F32 = jnp.float32
VMEM = pl.BlockSpec(memory_space=pltpu.VMEM)
SMEM = pl.BlockSpec(memory_space=pltpu.SMEM)
HBM = pl.BlockSpec(memory_space=pltpu.HBM)


def call(body, outs, args, smem=1, flops=0, scratch=(), vmem=8, hbm=(), far=False):
    args = [
        pltpu.with_memory_space_constraint(a, pltpu.HBM) if i in hbm else a
        for i, a in enumerate(args)
    ]
    moved = sum(a.size * a.dtype.itemsize for a in args) + sum(
        math.prod(o.shape) * o.dtype.itemsize for o in outs
    )
    return pl.pallas_call(
        body,
        out_shape=tuple(outs),
        in_specs=[SMEM if i < smem else HBM if i in hbm else VMEM for i in range(len(args))],
        out_specs=tuple([HBM if far else VMEM] * len(outs)),
        scratch_shapes=list(scratch),
        cost_estimate=pl.CostEstimate(flops=flops, transcendentals=0, bytes_accessed=moved),
        compiler_params=pltpu.CompilerParams(vmem_limit_bytes=vmem * 1024 * 1024),
    )(*args)


def shape(dims, dtype=BF):
    return jax.ShapeDtypeStruct(dims, dtype)


def nt(a, b):
    return lax.dot_general(a, b, (((1,), (1,)), ((), ())), preferred_element_type=F32)


def tn(a, b):
    return lax.dot_general(a, b, (((0,), (0,)), ((), ())), preferred_element_type=F32)


def routing(n_sp, nx, z, x, ids, wts):
    nz = n_sp // nx
    tok = ids.shape[1]
    first = lax.broadcasted_iota(jnp.int32, (n_sp, tok), 0)
    rz, rx = first // nx, first % nx
    zz, xx = rz + z, rx + x
    zz = jnp.where(zz >= nz, zz - nz, zz)
    xx = jnp.where(xx >= nx, xx - nx, xx)
    expert = zz * nx + xx
    hit0, hit1 = ids[0:1, :] == expert, ids[1:2, :] == expert
    named = jnp.where(hit0 | hit1, 1.0, 0.0)
    weight = 0.0
    if wts is not None:
        weight = jnp.where(hit0, wts[0:1, :], 0.0) + jnp.where(hit1, wts[1:2, :], 0.0)
    earlier = (
        lax.broadcasted_iota(jnp.int32, (tok, tok), 0)
        < lax.broadcasted_iota(jnp.int32, (tok, tok), 1)
    )
    before = jnp.dot(
        named.astype(BF), jnp.where(earlier, 1.0, 0.0).astype(BF), preferred_element_type=F32
    )
    return jnp.where(named > 0.5, before, -1.0), weight


def select_body(n_sp, nx, cap, me_ref, ids_ref, sel_ref):
    slot, _ = routing(n_sp, nx, me_ref[0], me_ref[1], ids_ref[...], None)
    place = lax.broadcasted_iota(jnp.int32, (cap, slot.shape[1]), 0).astype(F32)
    for r in range(n_sp):
        take = jnp.where(slot[r : r + 1, :] == place, 1.0, 0.0)
        sel_ref[r * cap : (r + 1) * cap, :] = take.astype(BF)


def dispatch_body(n_sp, nx, cap, me_ref, *refs):
    far, outs, near, sems = refs[:4], refs[4 : 4 + n_sp], refs[4 + n_sp : 8 + n_sp], refs[-1]
    copies = [pltpu.make_async_copy(f, n, sems.at[i]) for i, (f, n) in enumerate(zip(far, near))]
    for copy in copies:
        copy.start()
    for copy in copies:
        copy.wait()
    ids_ref, w_ref, x_ref, og_ref = near
    slot, weight = routing(n_sp, nx, me_ref[0], me_ref[1], ids_ref[...], w_ref[...])
    tok = x_ref.shape[0]
    place = lax.broadcasted_iota(jnp.int32, (cap, tok), 0).astype(F32)
    xv, og = x_ref[...], og_ref[...]
    for r in range(n_sp):
        take = jnp.where(slot[r : r + 1, :] == place, 1.0, 0.0)
        scale = jnp.sum(take * weight[r : r + 1, :], axis=1, keepdims=True)
        take = take.astype(BF)
        outs[r][:cap, :] = jnp.dot(take, xv, preferred_element_type=F32).astype(BF)
        outs[r][cap:, :] = (scale * jnp.dot(take, og, preferred_element_type=F32)).astype(BF)


def rows_of(refs, cap, which):
    return jnp.concatenate(
        [
            ref[at + which * cap : at + (which + 1) * cap, :]
            for ref in refs
            for at in range(0, ref.shape[0], 2 * cap)
        ],
        axis=0,
    )


def load_body(wg, wu, wd, wg_out, wu_out, wd_out, sems):
    pairs = [(wg, wg_out), (wu, wu_out), (wd, wd_out)]
    rows = wg.shape[0]
    step = -(-rows // 8 // LOAD_CUTS) * 8
    copies = []
    for f, n in pairs:
        for at in range(0, rows, step):
            cut = pl.ds(at, min(step, rows - at))
            copies.append(
                pltpu.make_async_copy(f.at[cut, :], n.at[cut, :], sems.at[len(copies)])
            )
    for copy in copies:
        copy.start()
    for copy in copies:
        copy.wait()


def fetch_body(n, *refs):
    copies = [pltpu.make_async_copy(refs[i], refs[n + i], refs[-1].at[i]) for i in range(n)]
    for copy in copies:
        copy.start()
    for copy in copies:
        copy.wait()


def mix_body(core_ref, gb, co, mixed_ref, gb_near, co_near, sems):
    copies = [
        pltpu.make_async_copy(gb, gb_near, sems.at[0]),
        pltpu.make_async_copy(co, co_near, sems.at[1]),
    ]
    for copy in copies:
        copy.start()
    for copy in copies:
        copy.wait()
    half = mixed_ref.shape[0] // 2
    for i in range(2):
        at = pl.multiple_of((core_ref[0] + i) % 2 * half, half)
        gb_half, co_half = gb_near[pl.ds(at, half), :], co_near[pl.ds(at, half), :]
        mixed_ref[i * half : (i + 1) * half, :] = (
            gb_half.astype(F32) * co_half.astype(F32)
        ).astype(BF)


def expert_body(n_b, n_g, cap, blk_ref, dst_ref, *refs):
    blocks, refs = refs[: n_b * n_g], refs[n_b * n_g :]
    wg, wu, wd, hid_ref, dg_ref, du_ref = refs[:6]
    outs = refs[6:]
    ch = blocks[0].shape[1]
    gate = up = dhid = None
    for b in range(n_b):
        cols = pl.ds(pl.multiple_of(blk_ref[b] * ch, ch), ch)
        xb, dyb = rows_of(blocks[b::n_b], cap, 0), rows_of(blocks[b::n_b], cap, 1)
        g, u, d = nt(xb, wg[:, cols]), nt(xb, wu[:, cols]), nt(dyb, wd[:, cols])
        gate = g if gate is None else gate + g
        up = u if up is None else up + u
        dhid = d if dhid is None else dhid + d
    sig = jax.nn.sigmoid(gate)
    act = gate * sig
    hid_ref[...] = (act * up).astype(BF)
    dg = (dhid * up * (sig * (1.0 + gate * (1.0 - sig)))).astype(BF)
    du = (dhid * act).astype(BF)
    dg_ref[...] = dg
    du_ref[...] = du
    for b in range(n_b):
        cols = pl.ds(pl.multiple_of(dst_ref[b] * ch, ch), ch)
        part = jnp.dot(dg, wg[:, cols], preferred_element_type=F32) + jnp.dot(
            du, wu[:, cols], preferred_element_type=F32
        )
        outs[b][...] = part.astype(BF)


def weight_grad_body(n_c, n_b, cap, which, blk_ref, *refs):
    lefts, rights, out, held, sems = refs[:n_c], refs[n_c:-3], refs[-3], refs[-2], refs[-1]
    ch = rights[0].shape[1]
    left = jnp.concatenate([l[...] for l in lefts], axis=0).T
    copies = []
    for b in range(n_b):
        total = jnp.dot(left, rows_of(rights[b::n_b], cap, which), preferred_element_type=F32)
        held[b, :, :] = total.astype(BF)
        cols = pl.ds(pl.multiple_of(blk_ref[b] * ch, ch), ch)
        copies.append(pltpu.make_async_copy(held.at[b], out.at[:, cols], sems.at[b]))
        copies[b].start()
    for copy in copies:
        copy.wait()


def join_body(*refs):
    at = 0
    for ref in refs[:-1]:
        refs[-1][at : at + ref.shape[0], :] = ref[...]
        at += ref.shape[0]


def add_body(n_out, *refs):
    ins, outs = refs[:-n_out], refs[-n_out:]
    for i in range(n_out):
        outs[i][...] = (ins[2 * i][...].astype(F32) + ins[2 * i + 1][...].astype(F32)).astype(BF)


def sum_split_body(n_in, *refs):
    ins, outs = refs[:n_in], refs[n_in:]
    rows = outs[0].shape[0]
    for i, out in enumerate(outs):
        total = None
        for ref in ins:
            v = ref[i * rows : (i + 1) * rows, :].astype(F32)
            total = v if total is None else total + v
        out[...] = total.astype(BF)


def combine_body(n_sp, sel_ref, og_ref, *refs):
    backs, dh_ref = refs[:n_sp], refs[n_sp]
    rows = jnp.concatenate([b[...] for b in backs], axis=0) if n_sp > 1 else backs[0][...]
    moe = tn(sel_ref[...], rows)
    dh_ref[...] = (og_ref[...].astype(F32) + moe).astype(BF)


def spread_body(n_b, n_sp, blk_ref, tgt_ref, core_ref, *refs):
    blocks, full_ref, outs = refs[:n_b], refs[n_b], refs[n_b + 1 :]
    ch = blocks[0].shape[1]
    for b in range(n_b):
        full_ref[:, pl.ds(pl.multiple_of(blk_ref[b] * ch, ch), ch)] = blocks[b][...]
    rows, w = full_ref.shape[0] // 2, outs[0].shape[1]
    nx, lane = len(outs), 128
    mine = pl.ds(pl.multiple_of(core_ref[0] * rows, rows), rows)
    for r in range(n_sp):
        out = outs[r % nx].at[r // nx * rows : (r // nx + 1) * rows, :]
        if w % lane == 0:
            out[...] = full_ref[mine, pl.ds(pl.multiple_of(tgt_ref[r] * w, lane), w)]
            continue
        fold = lane // w
        wide = full_ref[mine, pl.ds(pl.multiple_of(tgt_ref[r] // fold * lane, lane), lane)]
        piece = wide[:, :w]
        for i in range(1, fold):
            piece = jnp.where(tgt_ref[r] % fold == i, wide[:, i * w : (i + 1) * w], piece)
        out[...] = piece


def regroup_body(nx, *refs):
    ins, outs = refs[:nx], refs[nx:]
    rows = outs[0].shape[0] // nx
    for rz, out in enumerate(outs):
        for rx, ref in enumerate(ins):
            out[rx * rows : (rx + 1) * rows, :] = ref[rz * rows : (rz + 1) * rows, :]


def mixer_body(n_b, full_ref, wo_far, gb_far, co_far, *refs):
    dconv_ref, grad_b_ref, first_ref, last_ref, wo, gb, co, sems = refs
    ch = wo.shape[0] // n_b
    copies = []
    for b in range(n_b):
        at = slice(b * ch, (b + 1) * ch)
        copies.append(pltpu.make_async_copy(wo_far.at[at, :], wo.at[at, :], sems.at[b]))
    copies.append(pltpu.make_async_copy(gb_far, gb, sems.at[n_b]))
    copies.append(pltpu.make_async_copy(co_far, co, sems.at[n_b + 1]))
    for copy in copies:
        copy.start()
    dz = None
    for b in range(n_b):
        at = slice(b * ch, (b + 1) * ch)
        copies[b].wait()
        part = jnp.dot(full_ref[:, at], wo[at, :], preferred_element_type=F32)
        dz = part if dz is None else dz + part
    copies[n_b].wait()
    copies[n_b + 1].wait()
    dconv = (dz * gb[...].astype(F32)).astype(BF)
    dconv_ref[...] = dconv
    grad_b_ref[...] = (dz * co[...].astype(F32)).astype(BF)
    rows = dconv.shape[0]
    first_ref[...] = dconv[0:1, :]
    last_ref[...] = dconv[rows - 1 : rows, :]


def conv_body(dconv_ref, low_ref, high_ref, taps_ref, v_ref, c_ref, gc_ref, gv_ref):
    mid = dconv_ref[...].astype(F32)
    rows = mid.shape[0]
    at = lax.broadcasted_iota(jnp.int32, mid.shape, 0)
    prev = jnp.where(at == 0, low_ref[...].astype(F32), pltpu.roll(mid, 1, 0))
    succ = jnp.where(at == rows - 1, high_ref[...].astype(F32), pltpu.roll(mid, rows - 1, 0))
    taps = taps_ref[...]
    du = taps[0:1, :] * succ + taps[1:2, :] * mid + taps[2:3, :] * prev
    gc_ref[...] = (du * v_ref[...].astype(F32)).astype(BF)
    gv_ref[...] = (du * c_ref[...].astype(F32)).astype(BF)


def grad_out_body(nz, nx, *refs):
    mine, other, mixed, out = refs[:nz], refs[nz : 2 * nz], refs[2 * nz : 3 * nz], refs[-1]
    half = mine[0].shape[0] // nx
    lefts, rights = [], []
    for which, held in enumerate((mine, other)):
        for left, right in zip(held, mixed):
            lefts.append(left[...])
            for rx in range(nx):
                rights.append(right[(2 * rx + which) * half : (2 * rx + which + 1) * half, :])
    out[...] = tn(jnp.concatenate(lefts, axis=0), jnp.concatenate(rights, axis=0))


def grid(n_sp, n_tp):
    ny = n_tp // 2
    nx = ny if n_sp % ny == 0 else 1
    return n_sp // nx, nx, ny


def local(
    out_grad,
    moe_input,
    route_weight,
    route_ids,
    gate_proj,
    up_proj,
    down_proj,
    out_proj,
    conv_out,
    gate_b,
    gate_c,
    value_v,
    conv_taps,
):
    tok, ch = out_grad.shape
    n_sp, n_tp = lax.axis_size("sp"), lax.axis_size("tp")
    cap = 4 * tok // n_sp
    nz, nx, ny = grid(n_sp, n_tp)
    me, mt = lax.axis_index("sp"), lax.axis_index("tp")
    z, x, y, c = me // nx, me % nx, mt // 2, mt % 2
    i32 = functools.partial(jnp.asarray, dtype=jnp.int32)

    def sp_perm(rz, rx):
        return [
            (i, ((i // nx + rz) % nz) * nx + (i % nx + rx) % nx) for i in range(n_sp)
        ]

    def send_sp(v, rz, rx):
        if rz % nz == 0 and rx % nx == 0:
            return v
        return lax.ppermute(v, "sp", sp_perm(rz, rx))

    def send_y(v, jy):
        return lax.ppermute(v, "tp", [(k, ((k // 2 + jy) % ny) * 2 + k % 2) for k in range(n_tp)])

    def send_core(v):
        return lax.ppermute(v, "tp", [(k, k ^ 1) for k in range(n_tp)])

    def gather_tp(v):
        blocks = []
        for jy in range(ny):
            b = send_y(v, jy) if jy else v
            blocks += [b, send_core(b)]
        return blocks

    rel = [(rz, rx) for rz in range(nz) for rx in range(nx)]
    blk = i32([0]) + jnp.stack(
        [((y - jy) % ny) * 2 + (c + cc) % 2 for jy in range(ny) for cc in range(2)]
    ).astype(jnp.int32)
    dst = jnp.stack(
        [((y + jy) % ny) * 2 + (c + cc) % 2 for jy in range(ny) for cc in range(2)]
    ).astype(jnp.int32)
    tgt = jnp.stack([((z + rz) % nz) * nx + (x + rx) % nx for rz, rx in rel]).astype(jnp.int32)

    near = [
        pltpu.VMEM((2, tok), jnp.int32), pltpu.VMEM((2, tok), F32),
        pltpu.VMEM((tok, ch), BF), pltpu.VMEM((tok, ch), BF), pltpu.SemaphoreType.DMA((4,)),
    ]
    at = jnp.stack([z, x]).astype(jnp.int32)
    sent = call(
        functools.partial(dispatch_body, n_sp, nx, cap),
        [shape((2 * cap, ch))] * n_sp,
        [at, route_ids.T, route_weight.T, moe_input, out_grad],
        flops=4 * n_sp * cap * tok * ch, scratch=near, hbm=(1, 2, 3, 4),
    )
    groups = []
    for rz in range(nz):
        got = [send_sp(sent[rz * nx + rx], rz, rx) for rx in range(nx)]
        if nx > 1:
            got = call(join_body, [shape((nx * 2 * cap, ch))], got, smem=0, flops=cap)
        groups.append(gather_tp(got[0]))

    core = c.reshape(1).astype(jnp.int32)

    ff = down_proj.shape[1]
    weights = [gate_proj[0].T, up_proj[0].T, down_proj[0]]
    mixed = call(
        mix_body, [shape((tok, ch))], [core, gate_b, conv_out], hbm=(1, 2),
        flops=tok * ch,
        scratch=[pltpu.VMEM((tok, ch), BF)] * 2 + [pltpu.SemaphoreType.DMA((2,))],
    )[0]
    weights = call(
        load_body, [shape((ff, ch * n_tp))] * 3, weights, smem=0, hbm=range(3),
        scratch=[pltpu.SemaphoreType.DMA((3 * LOAD_CUTS,))],
    )
    row = [send_sp(mixed, 0, rx) for rx in range(nx)]
    row = call(join_body, [shape((nx * tok, ch))], row, smem=0, flops=tok)[0]
    mixed_all = [row]
    for _ in range(1, nz):
        row = send_sp(row, 1, 0)
        mixed_all.append(row)

    n_c = 2 if nz % 2 == 0 else 1
    gpc, per = nz // n_c, n_sp // n_c
    rows = per * cap
    hid, dgs, dus, backs = [], [], [], []
    for g in range(n_c):
        outs = call(
            functools.partial(expert_body, n_tp, gpc, cap),
            [shape((rows, ff))] * 3 + [shape((rows, ch))] * n_tp,
            [blk, dst, *[b for group in groups[g * gpc : (g + 1) * gpc] for b in group],
             *weights],
            smem=2, vmem=EXPERT_MIB,
            flops=10 * rows * ff * ch * n_tp,
        )
        blk = lax.optimization_barrier((blk, outs[0]))[0]
        hid.append(outs[0])
        dgs.append(outs[1])
        dus.append(outs[2])
        parts = outs[3:]
        theirs = [send_core(parts[2 * jy + 1]) for jy in range(ny)]
        pairs = [v for jy in range(ny) for v in (parts[2 * jy], theirs[jy])]
        summed = call(
            functools.partial(add_body, ny), [shape((rows, ch))] * ny, pairs, smem=0,
            flops=ny * rows * ch,
        )
        arrived = [summed[0]] + [send_y(summed[jy], jy) for jy in range(1, ny)]
        pieces = call(
            functools.partial(sum_split_body, ny), [shape((cap, ch))] * per, arrived,
            smem=0, flops=ny * rows * ch,
        )
        for i, (rz, rx) in enumerate(rel[g * per : (g + 1) * per]):
            backs.append(send_sp(pieces[i], -rz, -rx))

    def weight_grad(lefts, which):
        return call(
            functools.partial(weight_grad_body, n_c, n_tp, cap, which),
            [pltpu.HBM((ff, ch * n_tp), BF)],
            [blk, *lefts, *[b for group in groups for b in group]],
            flops=2 * n_sp * cap * ff * ch * n_tp, vmem=GRAD_MIB, far=True,
            scratch=[pltpu.VMEM((n_tp, ff, ch), BF), pltpu.SemaphoreType.DMA((n_tp,))],
        )[0]

    grad_down = weight_grad(hid, 1)
    grad_gate = weight_grad(dgs, 0)
    grad_up = weight_grad(dus, 0)
    grad_gate, grad_up = grad_gate.T, grad_up.T

    sel = call(
        functools.partial(select_body, n_sp, nx, cap), [shape((n_sp * cap, tok))],
        [at, route_ids.T], flops=2 * n_sp * cap * tok * tok,
    )[0]
    dh = call(
        functools.partial(combine_body, n_sp), [shape((tok, ch))],
        [sel, out_grad, *backs], smem=0, flops=2 * n_sp * cap * tok * ch,
    )[0]
    dh_blocks = gather_tp(dh)
    width, half = ch * n_tp // n_sp, tok // 2
    outs = call(
        functools.partial(spread_body, n_tp, n_sp),
        [shape((tok, ch * n_tp))] + [shape((nz * half, width))] * nx,
        [blk, tgt, core, *dh_blocks], smem=3, flops=tok * ch * n_tp,
    )
    full_h, slices = outs[0], outs[1:]
    slices = [send_sp(slices[rx], 0, rx) for rx in range(nx)]
    slices = call(
        functools.partial(regroup_body, nx), [shape((nx * half, width))] * nz, slices,
        smem=0, flops=tok * width,
    )
    dh_mine = [send_sp(slices[rz], rz, 0) for rz in range(nz)]
    dh_other = [send_core(v) for v in dh_mine]

    dconv, grad_b, first, last = call(
        functools.partial(mixer_body, n_tp), [shape((tok, ch)), shape((tok, ch)), shape((1, ch)), shape((1, ch))],
        [full_h, out_proj, gate_b, conv_out], smem=0, flops=2 * tok * ch * ch * n_tp, hbm=(1, 2, 3),
        scratch=[
            pltpu.VMEM(out_proj.shape, BF), pltpu.VMEM((tok, ch), BF), pltpu.VMEM((tok, ch), BF),
            pltpu.SemaphoreType.DMA((n_tp + 2,)),
        ],
    )
    up_pairs = [(i, i + 1) for i in range(n_sp - 1)]
    low = lax.ppermute(last, "sp", up_pairs)
    high = lax.ppermute(first, "sp", [(b, a) for a, b in up_pairs])
    grad_c, grad_v = call(
        conv_body, [shape((tok, ch))] * 2,
        [dconv, low, high, conv_taps, value_v, gate_c], smem=0, flops=8 * tok * ch,
    )
    mixed_all = call(
        functools.partial(fetch_body, nz), [shape((nx * tok, ch))] * nz, mixed_all,
        smem=0, hbm=range(nz), scratch=[pltpu.SemaphoreType.DMA((nz,))],
    )
    grad_out = call(
        functools.partial(grad_out_body, nz, nx), [shape((width, ch), F32)],
        [*dh_mine, *dh_other, *mixed_all], smem=0, flops=2 * n_sp * tok * width * ch,
    )[0]
    return (grad_gate[None], grad_up[None], grad_down[None], grad_out, grad_b, grad_c, grad_v)


def solution(mesh):
    in_specs = (
        P("sp", "tp"),
        P("sp", "tp"),
        P("sp", None),
        P("sp", None),
        P("sp", None, "tp"),
        P("sp", None, "tp"),
        P("sp", "tp", None),
        P(None, "tp"),
        P("sp", "tp"),
        P("sp", "tp"),
        P("sp", "tp"),
        P("sp", "tp"),
        P(None, "tp"),
    )
    out_specs = (
        P("sp", None, "tp"),
        P("sp", None, "tp"),
        P("sp", "tp", None),
        P("sp", "tp"),
        P("sp", "tp"),
        P("sp", "tp"),
        P("sp", "tp"),
    )
    return jax.shard_map(local, mesh=mesh, in_specs=in_specs, out_specs=out_specs, check_vma=False)
```

```python
import functools
import math

import jax
import jax.numpy as jnp
from jax import lax
from jax.experimental import pallas as pl
from jax.experimental.pallas import tpu as pltpu
from jax.sharding import PartitionSpec as P


EXPERT_MIB, GRAD_MIB = 16, 14
LOAD_CUTS = 4
BF = jnp.bfloat16
F32 = jnp.float32
VMEM = pl.BlockSpec(memory_space=pltpu.VMEM)
SMEM = pl.BlockSpec(memory_space=pltpu.SMEM)
HBM = pl.BlockSpec(memory_space=pltpu.HBM)


def call(body, outs, args, smem=1, flops=0, scratch=(), vmem=8, hbm=(), far=False):
    args = [
        pltpu.with_memory_space_constraint(a, pltpu.HBM) if i in hbm else a
        for i, a in enumerate(args)
    ]
    moved = sum(a.size * a.dtype.itemsize for a in args) + sum(
        math.prod(o.shape) * o.dtype.itemsize for o in outs
    )
    return pl.pallas_call(
        body,
        out_shape=tuple(outs),
        in_specs=[SMEM if i < smem else HBM if i in hbm else VMEM for i in range(len(args))],
        out_specs=tuple([HBM if far else VMEM] * len(outs)),
        scratch_shapes=list(scratch),
        cost_estimate=pl.CostEstimate(flops=flops, transcendentals=0, bytes_accessed=moved),
        compiler_params=pltpu.CompilerParams(vmem_limit_bytes=vmem * 1024 * 1024),
    )(*args)


def shape(dims, dtype=BF):
    return jax.ShapeDtypeStruct(dims, dtype)


def nt(a, b):
    return lax.dot_general(a, b, (((1,), (1,)), ((), ())), preferred_element_type=F32)


def tn(a, b):
    return lax.dot_general(a, b, (((0,), (0,)), ((), ())), preferred_element_type=F32)


def routing(n_sp, nx, z, x, ids, wts):
    nz = n_sp // nx
    tok = ids.shape[1]
    first = lax.broadcasted_iota(jnp.int32, (n_sp, tok), 0)
    rz, rx = first // nx, first % nx
    zz, xx = rz + z, rx + x
    zz = jnp.where(zz >= nz, zz - nz, zz)
    xx = jnp.where(xx >= nx, xx - nx, xx)
    expert = zz * nx + xx
    hit0, hit1 = ids[0:1, :] == expert, ids[1:2, :] == expert
    named = jnp.where(hit0 | hit1, 1.0, 0.0)
    weight = 0.0
    if wts is not None:
        weight = jnp.where(hit0, wts[0:1, :], 0.0) + jnp.where(hit1, wts[1:2, :], 0.0)
    earlier = (
        lax.broadcasted_iota(jnp.int32, (tok, tok), 0)
        < lax.broadcasted_iota(jnp.int32, (tok, tok), 1)
    )
    before = jnp.dot(
        named.astype(BF), jnp.where(earlier, 1.0, 0.0).astype(BF), preferred_element_type=F32
    )
    return jnp.where(named > 0.5, before, -1.0), weight


def select_body(n_sp, nx, cap, me_ref, ids_ref, sel_ref):
    slot, _ = routing(n_sp, nx, me_ref[0], me_ref[1], ids_ref[...], None)
    place = lax.broadcasted_iota(jnp.int32, (cap, slot.shape[1]), 0).astype(F32)
    for r in range(n_sp):
        take = jnp.where(slot[r : r + 1, :] == place, 1.0, 0.0)
        sel_ref[r * cap : (r + 1) * cap, :] = take.astype(BF)


def dispatch_body(n_sp, nx, cap, me_ref, *refs):
    far, outs, near, sems = refs[:4], refs[4 : 4 + n_sp], refs[4 + n_sp : 8 + n_sp], refs[-1]
    copies = [pltpu.make_async_copy(f, n, sems.at[i]) for i, (f, n) in enumerate(zip(far, near))]
    for copy in copies:
        copy.start()
    for copy in copies:
        copy.wait()
    ids_ref, w_ref, x_ref, og_ref = near
    slot, weight = routing(n_sp, nx, me_ref[0], me_ref[1], ids_ref[...], w_ref[...])
    tok = x_ref.shape[0]
    place = lax.broadcasted_iota(jnp.int32, (cap, tok), 0).astype(F32)
    xv, og = x_ref[...], og_ref[...]
    for r in range(n_sp):
        take = jnp.where(slot[r : r + 1, :] == place, 1.0, 0.0)
        scale = jnp.sum(take * weight[r : r + 1, :], axis=1, keepdims=True)
        take = take.astype(BF)
        outs[r][:cap, :] = jnp.dot(take, xv, preferred_element_type=F32).astype(BF)
        outs[r][cap:, :] = (scale * jnp.dot(take, og, preferred_element_type=F32)).astype(BF)


def rows_of(refs, cap, which):
    return jnp.concatenate(
        [
            ref[at + which * cap : at + (which + 1) * cap, :]
            for ref in refs
            for at in range(0, ref.shape[0], 2 * cap)
        ],
        axis=0,
    )


def load_body(n_row, wg, wu, wd, *refs):
    rows_in, (wg_out, wu_out, wd_out, joined, sems) = refs[:n_row], refs[n_row:]
    rows, tok = wg.shape[0], joined.shape[0] // n_row
    step = -(-rows // 8 // LOAD_CUTS) * 8
    pairs = [(ref, joined.at[i * tok : (i + 1) * tok, :]) for i, ref in enumerate(rows_in)]
    for f, n in ((wg, wg_out), (wu, wu_out), (wd, wd_out)):
        for at in range(0, rows, step):
            cut = pl.ds(at, min(step, rows - at))
            pairs.append((f.at[cut, :], n.at[cut, :]))
    copies = [pltpu.make_async_copy(f, n, sems.at[i]) for i, (f, n) in enumerate(pairs)]
    for copy in copies:
        copy.start()
    for copy in copies:
        copy.wait()


def fetch_body(n, *refs):
    copies = [pltpu.make_async_copy(refs[i], refs[n + i], refs[-1].at[i]) for i in range(n)]
    for copy in copies:
        copy.start()
    for copy in copies:
        copy.wait()


def mix_body(core_ref, gb, co, mixed_ref, gb_near, co_near, sems):
    copies = [
        pltpu.make_async_copy(gb, gb_near, sems.at[0]),
        pltpu.make_async_copy(co, co_near, sems.at[1]),
    ]
    for copy in copies:
        copy.start()
    for copy in copies:
        copy.wait()
    half = mixed_ref.shape[0] // 2
    for i in range(2):
        at = pl.multiple_of((core_ref[0] + i) % 2 * half, half)
        gb_half, co_half = gb_near[pl.ds(at, half), :], co_near[pl.ds(at, half), :]
        mixed_ref[i * half : (i + 1) * half, :] = (
            gb_half.astype(F32) * co_half.astype(F32)
        ).astype(BF)


def expert_body(n_b, n_g, cap, blk_ref, dst_ref, *refs):
    blocks, refs = refs[: n_b * n_g], refs[n_b * n_g :]
    wg, wu, wd, hid_ref, dg_ref, du_ref = refs[:6]
    outs = refs[6:]
    ch = blocks[0].shape[1]
    gate = up = dhid = None
    for b in range(n_b):
        cols = pl.ds(pl.multiple_of(blk_ref[b] * ch, ch), ch)
        xb, dyb = rows_of(blocks[b::n_b], cap, 0), rows_of(blocks[b::n_b], cap, 1)
        g, u, d = nt(xb, wg[:, cols]), nt(xb, wu[:, cols]), nt(dyb, wd[:, cols])
        gate = g if gate is None else gate + g
        up = u if up is None else up + u
        dhid = d if dhid is None else dhid + d
    sig = jax.nn.sigmoid(gate)
    act = gate * sig
    hid_ref[...] = (act * up).astype(BF)
    dg = (dhid * up * (sig * (1.0 + gate * (1.0 - sig)))).astype(BF)
    du = (dhid * act).astype(BF)
    dg_ref[...] = dg
    du_ref[...] = du
    for b in range(n_b):
        cols = pl.ds(pl.multiple_of(dst_ref[b] * ch, ch), ch)
        part = jnp.dot(dg, wg[:, cols], preferred_element_type=F32) + jnp.dot(
            du, wu[:, cols], preferred_element_type=F32
        )
        outs[b][...] = part.astype(BF)


def weight_grad_body(n_c, n_b, cap, which, blk_ref, *refs):
    lefts, rights, out, held, sems = refs[:n_c], refs[n_c:-3], refs[-3], refs[-2], refs[-1]
    ch = rights[0].shape[1]
    left = jnp.concatenate([l[...] for l in lefts], axis=0).T
    copies = []
    for b in range(n_b):
        total = jnp.dot(left, rows_of(rights[b::n_b], cap, which), preferred_element_type=F32)
        held[b, :, :] = total.astype(BF)
        cols = pl.ds(pl.multiple_of(blk_ref[b] * ch, ch), ch)
        copies.append(pltpu.make_async_copy(held.at[b], out.at[:, cols], sems.at[b]))
        copies[b].start()
    for copy in copies:
        copy.wait()


def join_body(*refs):
    at = 0
    for ref in refs[:-1]:
        refs[-1][at : at + ref.shape[0], :] = ref[...]
        at += ref.shape[0]


def add_body(n_out, *refs):
    ins, outs = refs[:-n_out], refs[-n_out:]
    for i in range(n_out):
        outs[i][...] = (ins[2 * i][...].astype(F32) + ins[2 * i + 1][...].astype(F32)).astype(BF)


def sum_split_body(n_in, *refs):
    ins, outs = refs[:n_in], refs[n_in:]
    rows = outs[0].shape[0]
    for i, out in enumerate(outs):
        total = None
        for ref in ins:
            v = ref[i * rows : (i + 1) * rows, :].astype(F32)
            total = v if total is None else total + v
        out[...] = total.astype(BF)


def combine_body(n_sp, sel_ref, og_ref, *refs):
    backs, dh_ref = refs[:n_sp], refs[n_sp]
    rows = jnp.concatenate([b[...] for b in backs], axis=0) if n_sp > 1 else backs[0][...]
    moe = tn(sel_ref[...], rows)
    dh_ref[...] = (og_ref[...].astype(F32) + moe).astype(BF)


def spread_body(n_b, n_sp, blk_ref, tgt_ref, core_ref, *refs):
    blocks, full_ref, outs = refs[:n_b], refs[n_b], refs[n_b + 1 :]
    ch = blocks[0].shape[1]
    for b in range(n_b):
        full_ref[:, pl.ds(pl.multiple_of(blk_ref[b] * ch, ch), ch)] = blocks[b][...]
    rows, w = full_ref.shape[0] // 2, outs[0].shape[1]
    nx, lane = len(outs), 128
    mine = pl.ds(pl.multiple_of(core_ref[0] * rows, rows), rows)
    for r in range(n_sp):
        out = outs[r % nx].at[r // nx * rows : (r // nx + 1) * rows, :]
        if w % lane == 0:
            out[...] = full_ref[mine, pl.ds(pl.multiple_of(tgt_ref[r] * w, lane), w)]
            continue
        fold = lane // w
        wide = full_ref[mine, pl.ds(pl.multiple_of(tgt_ref[r] // fold * lane, lane), lane)]
        piece = wide[:, :w]
        for i in range(1, fold):
            piece = jnp.where(tgt_ref[r] % fold == i, wide[:, i * w : (i + 1) * w], piece)
        out[...] = piece


def regroup_body(nx, *refs):
    ins, outs = refs[:nx], refs[nx:]
    rows = outs[0].shape[0] // nx
    for rz, out in enumerate(outs):
        for rx, ref in enumerate(ins):
            out[rx * rows : (rx + 1) * rows, :] = ref[rz * rows : (rz + 1) * rows, :]


def mixer_body(n_b, full_ref, wo_far, gb_far, co_far, *refs):
    dconv_ref, grad_b_ref, first_ref, last_ref, wo, gb, co, sems = refs
    ch = wo.shape[0] // n_b
    copies = []
    for b in range(n_b):
        at = slice(b * ch, (b + 1) * ch)
        copies.append(pltpu.make_async_copy(wo_far.at[at, :], wo.at[at, :], sems.at[b]))
    copies.append(pltpu.make_async_copy(gb_far, gb, sems.at[n_b]))
    copies.append(pltpu.make_async_copy(co_far, co, sems.at[n_b + 1]))
    for copy in copies:
        copy.start()
    dz = None
    for b in range(n_b):
        at = slice(b * ch, (b + 1) * ch)
        copies[b].wait()
        part = jnp.dot(full_ref[:, at], wo[at, :], preferred_element_type=F32)
        dz = part if dz is None else dz + part
    copies[n_b].wait()
    copies[n_b + 1].wait()
    dconv = (dz * gb[...].astype(F32)).astype(BF)
    dconv_ref[...] = dconv
    grad_b_ref[...] = (dz * co[...].astype(F32)).astype(BF)
    rows = dconv.shape[0]
    first_ref[...] = dconv[0:1, :]
    last_ref[...] = dconv[rows - 1 : rows, :]


def conv_body(dconv_ref, low_ref, high_ref, taps_ref, v_ref, c_ref, gc_ref, gv_ref):
    mid = dconv_ref[...].astype(F32)
    rows = mid.shape[0]
    at = lax.broadcasted_iota(jnp.int32, mid.shape, 0)
    prev = jnp.where(at == 0, low_ref[...].astype(F32), pltpu.roll(mid, 1, 0))
    succ = jnp.where(at == rows - 1, high_ref[...].astype(F32), pltpu.roll(mid, rows - 1, 0))
    taps = taps_ref[...]
    du = taps[0:1, :] * succ + taps[1:2, :] * mid + taps[2:3, :] * prev
    gc_ref[...] = (du * v_ref[...].astype(F32)).astype(BF)
    gv_ref[...] = (du * c_ref[...].astype(F32)).astype(BF)


def grad_out_body(nz, nx, *refs):
    mine, other, mixed, out = refs[:nz], refs[nz : 2 * nz], refs[2 * nz : 3 * nz], refs[-1]
    half = mine[0].shape[0] // nx
    lefts, rights = [], []
    for which, held in enumerate((mine, other)):
        for left, right in zip(held, mixed):
            lefts.append(left[...])
            for rx in range(nx):
                rights.append(right[(2 * rx + which) * half : (2 * rx + which + 1) * half, :])
    out[...] = tn(jnp.concatenate(lefts, axis=0), jnp.concatenate(rights, axis=0))


def grid(n_sp, n_tp):
    ny = n_tp // 2
    nx = ny if n_sp % ny == 0 else 1
    return n_sp // nx, nx, ny


def local(
    out_grad,
    moe_input,
    route_weight,
    route_ids,
    gate_proj,
    up_proj,
    down_proj,
    out_proj,
    conv_out,
    gate_b,
    gate_c,
    value_v,
    conv_taps,
):
    tok, ch = out_grad.shape
    n_sp, n_tp = lax.axis_size("sp"), lax.axis_size("tp")
    cap = 4 * tok // n_sp
    nz, nx, ny = grid(n_sp, n_tp)
    me, mt = lax.axis_index("sp"), lax.axis_index("tp")
    z, x, y, c = me // nx, me % nx, mt // 2, mt % 2
    i32 = functools.partial(jnp.asarray, dtype=jnp.int32)

    def sp_perm(rz, rx):
        return [
            (i, ((i // nx + rz) % nz) * nx + (i % nx + rx) % nx) for i in range(n_sp)
        ]

    def send_sp(v, rz, rx):
        if rz % nz == 0 and rx % nx == 0:
            return v
        return lax.ppermute(v, "sp", sp_perm(rz, rx))

    def send_y(v, jy):
        return lax.ppermute(v, "tp", [(k, ((k // 2 + jy) % ny) * 2 + k % 2) for k in range(n_tp)])

    def send_core(v):
        return lax.ppermute(v, "tp", [(k, k ^ 1) for k in range(n_tp)])

    def gather_tp(v):
        blocks = []
        for jy in range(ny):
            b = send_y(v, jy) if jy else v
            blocks += [b, send_core(b)]
        return blocks

    rel = [(rz, rx) for rz in range(nz) for rx in range(nx)]
    blk = i32([0]) + jnp.stack(
        [((y - jy) % ny) * 2 + (c + cc) % 2 for jy in range(ny) for cc in range(2)]
    ).astype(jnp.int32)
    dst = jnp.stack(
        [((y + jy) % ny) * 2 + (c + cc) % 2 for jy in range(ny) for cc in range(2)]
    ).astype(jnp.int32)
    tgt = jnp.stack([((z + rz) % nz) * nx + (x + rx) % nx for rz, rx in rel]).astype(jnp.int32)

    near = [
        pltpu.VMEM((2, tok), jnp.int32), pltpu.VMEM((2, tok), F32),
        pltpu.VMEM((tok, ch), BF), pltpu.VMEM((tok, ch), BF), pltpu.SemaphoreType.DMA((4,)),
    ]
    at = jnp.stack([z, x]).astype(jnp.int32)
    sent = call(
        functools.partial(dispatch_body, n_sp, nx, cap),
        [shape((2 * cap, ch))] * n_sp,
        [at, route_ids.T, route_weight.T, moe_input, out_grad],
        flops=4 * n_sp * cap * tok * ch, scratch=near, hbm=(1, 2, 3, 4),
    )
    groups = []
    for rz in range(nz):
        got = [send_sp(sent[rz * nx + rx], rz, rx) for rx in range(nx)]
        if nx > 1:
            got = call(join_body, [shape((nx * 2 * cap, ch))], got, smem=0, flops=cap)
        groups.append(gather_tp(got[0]))

    core = c.reshape(1).astype(jnp.int32)

    ff = down_proj.shape[1]
    weights = [gate_proj[0].T, up_proj[0].T, down_proj[0]]
    mixed = call(
        mix_body, [shape((tok, ch))], [core, gate_b, conv_out], hbm=(1, 2),
        flops=tok * ch,
        scratch=[pltpu.VMEM((tok, ch), BF)] * 2 + [pltpu.SemaphoreType.DMA((2,))],
    )[0]
    row = [send_sp(mixed, 0, rx) for rx in range(nx)]
    *weights, row = call(
        functools.partial(load_body, nx),
        [shape((ff, ch * n_tp))] * 3 + [shape((nx * tok, ch))], [*weights, *row], smem=0,
        hbm=range(3 + nx), scratch=[pltpu.SemaphoreType.DMA((3 * LOAD_CUTS + nx,))],
    )
    mixed_all = [row]
    for _ in range(1, nz):
        row = send_sp(row, 1, 0)
        mixed_all.append(row)

    n_c = 2 if nz % 2 == 0 else 1
    gpc, per = nz // n_c, n_sp // n_c
    rows = per * cap
    hid, dgs, dus, backs = [], [], [], []
    for g in range(n_c):
        outs = call(
            functools.partial(expert_body, n_tp, gpc, cap),
            [shape((rows, ff))] * 3 + [shape((rows, ch))] * n_tp,
            [blk, dst, *[b for group in groups[g * gpc : (g + 1) * gpc] for b in group],
             *weights],
            smem=2, vmem=EXPERT_MIB,
            flops=10 * rows * ff * ch * n_tp,
        )
        blk = lax.optimization_barrier((blk, outs[0]))[0]
        hid.append(outs[0])
        dgs.append(outs[1])
        dus.append(outs[2])
        parts = outs[3:]
        theirs = [send_core(parts[2 * jy + 1]) for jy in range(ny)]
        pairs = [v for jy in range(ny) for v in (parts[2 * jy], theirs[jy])]
        summed = call(
            functools.partial(add_body, ny), [shape((rows, ch))] * ny, pairs, smem=0,
            flops=ny * rows * ch,
        )
        arrived = [summed[0]] + [send_y(summed[jy], jy) for jy in range(1, ny)]
        pieces = call(
            functools.partial(sum_split_body, ny), [shape((cap, ch))] * per, arrived,
            smem=0, flops=ny * rows * ch,
        )
        for i, (rz, rx) in enumerate(rel[g * per : (g + 1) * per]):
            backs.append(send_sp(pieces[i], -rz, -rx))

    def weight_grad(lefts, which):
        return call(
            functools.partial(weight_grad_body, n_c, n_tp, cap, which),
            [pltpu.HBM((ff, ch * n_tp), BF)],
            [blk, *lefts, *[b for group in groups for b in group]],
            flops=2 * n_sp * cap * ff * ch * n_tp, vmem=GRAD_MIB, far=True,
            scratch=[pltpu.VMEM((n_tp, ff, ch), BF), pltpu.SemaphoreType.DMA((n_tp,))],
        )[0]

    grad_down = weight_grad(hid, 1)
    grad_gate = weight_grad(dgs, 0)
    grad_up = weight_grad(dus, 0)
    grad_gate, grad_up = grad_gate.T, grad_up.T

    sel = call(
        functools.partial(select_body, n_sp, nx, cap), [shape((n_sp * cap, tok))],
        [at, route_ids.T], flops=2 * n_sp * cap * tok * tok,
    )[0]
    dh = call(
        functools.partial(combine_body, n_sp), [shape((tok, ch))],
        [sel, out_grad, *backs], smem=0, flops=2 * n_sp * cap * tok * ch,
    )[0]
    dh_blocks = gather_tp(dh)
    width, half = ch * n_tp // n_sp, tok // 2
    outs = call(
        functools.partial(spread_body, n_tp, n_sp),
        [shape((tok, ch * n_tp))] + [shape((nz * half, width))] * nx,
        [blk, tgt, core, *dh_blocks], smem=3, flops=tok * ch * n_tp,
    )
    full_h, slices = outs[0], outs[1:]
    slices = [send_sp(slices[rx], 0, rx) for rx in range(nx)]
    slices = call(
        functools.partial(regroup_body, nx), [shape((nx * half, width))] * nz, slices,
        smem=0, flops=tok * width,
    )
    dh_mine = [send_sp(slices[rz], rz, 0) for rz in range(nz)]
    dh_other = [send_core(v) for v in dh_mine]

    dconv, grad_b, first, last = call(
        functools.partial(mixer_body, n_tp), [shape((tok, ch)), shape((tok, ch)), shape((1, ch)), shape((1, ch))],
        [full_h, out_proj, gate_b, conv_out], smem=0, flops=2 * tok * ch * ch * n_tp, hbm=(1, 2, 3),
        scratch=[
            pltpu.VMEM(out_proj.shape, BF), pltpu.VMEM((tok, ch), BF), pltpu.VMEM((tok, ch), BF),
            pltpu.SemaphoreType.DMA((n_tp + 2,)),
        ],
    )
    up_pairs = [(i, i + 1) for i in range(n_sp - 1)]
    low = lax.ppermute(last, "sp", up_pairs)
    high = lax.ppermute(first, "sp", [(b, a) for a, b in up_pairs])
    grad_c, grad_v = call(
        conv_body, [shape((tok, ch))] * 2,
        [dconv, low, high, conv_taps, value_v, gate_c], smem=0, flops=8 * tok * ch,
    )
    mixed_all = call(
        functools.partial(fetch_body, nz), [shape((nx * tok, ch))] * nz, mixed_all,
        smem=0, hbm=range(nz), scratch=[pltpu.SemaphoreType.DMA((nz,))],
    )
    grad_out = call(
        functools.partial(grad_out_body, nz, nx), [shape((width, ch), F32)],
        [*dh_mine, *dh_other, *mixed_all], smem=0, flops=2 * n_sp * tok * width * ch,
    )[0]
    return (grad_gate[None], grad_up[None], grad_down[None], grad_out, grad_b, grad_c, grad_v)


def solution(mesh):
    in_specs = (
        P("sp", "tp"),
        P("sp", "tp"),
        P("sp", None),
        P("sp", None),
        P("sp", None, "tp"),
        P("sp", None, "tp"),
        P("sp", "tp", None),
        P(None, "tp"),
        P("sp", "tp"),
        P("sp", "tp"),
        P("sp", "tp"),
        P("sp", "tp"),
        P(None, "tp"),
    )
    out_specs = (
        P("sp", None, "tp"),
        P("sp", None, "tp"),
        P("sp", "tp", None),
        P("sp", "tp"),
        P("sp", "tp"),
        P("sp", "tp"),
        P("sp", "tp"),
    )
    return jax.shard_map(local, mesh=mesh, in_specs=in_specs, out_specs=out_specs, check_vma=False)
```
